32 devices in a mesh: sp: 16 (over z, y, core), tp: 2 (over x).
Axes of the slice: x: 2, y: 2, z: 4, core: 2. Of those that a mesh axis runs over, the one named last changes fastest.
Arguments:
- queries: bfloat16 [3072, 1024], P('sp', 'tp'), may hold values from -6 to 6
- keys: bfloat16 [3072, 512], P('sp', 'tp'), may hold values from -6 to 6
- values: bfloat16 [3072, 512], P('sp', 'tp'), may hold values from -6 to 6
- q_gain: float32 [64], replicated, may hold values from 0.1 to 6.5
- k_gain: float32 [64], replicated, may hold values from 0.1 to 6.5
- w_out: bfloat16 [1024, 2048], P('tp'), may hold values from -12 to 12
- residual: bfloat16 [3072, 2048], P(('sp', 'tp')), may hold values from -6 to 6
- norm_gain: float32 [2048], replicated, may hold values from 0.1 to 1.9
- w_gate: bfloat16 [2048, 5632], P('sp', 'tp'), may hold values from -0.125 to 0.125
- w_up: bfloat16 [2048, 5632], P('sp', 'tp'), may hold values from -0.125 to 0.125
- w_down: bfloat16 [5632, 2048], P('tp', 'sp'), may hold values from -0.25 to 0.25
Outputs:
- layer_out: bfloat16 [3072, 2048], P(('sp', 'tp'))
The draws below stay inside these ranges and needn't reach their ends.
All inputs are finite; a program needn't handle non-finite values.
Results may differ from the reference program's by a relative error of at most 0.018.
The reference program's roundings to bfloat16 on the way count: a program that leaves them out, or rounds other values in their place, can miss the bound.
Values may be sent and summed in bfloat16 or wider, within the bound.
No kernel may reach another device: no remote copies, remote signals or barrier semaphores. Data moves between devices by JAX's collectives and lax.ppermute only.
A program may use at most 128 MiB of HBM per device.

```python
import math
import jax
import jax.numpy as jnp
from jax import lax

D = 2048
FF = 5632
HEADS = 16
KV_HEADS = 8
HEAD = 64
GRID_W = 128
TOKENS = 3072
ATTN = 1024
KV_WIDTH = 512


def draw_queries(key, part):
    base = jnp.clip(jax.random.normal(jax.random.fold_in(key, 11), (TOKENS, HEADS * HEAD), jnp.float32), -6.0, 6.0)
    return base.astype(jnp.bfloat16)


def draw_keys(key, part):
    base = jnp.clip(jax.random.normal(jax.random.fold_in(key, 23), (TOKENS, KV_HEADS * HEAD), jnp.float32), -6.0, 6.0)
    return base.astype(jnp.bfloat16)


def draw_q_gain(key, part):
    return jax.random.uniform(jax.random.fold_in(key, 53), (HEAD,), jnp.float32, 0.1, 1.9)


def draw_k_gain(key, part):
    return jax.random.uniform(jax.random.fold_in(key, 63), (HEAD,), jnp.float32, 0.1, 1.9)


def draw_w_out(key, part):
    base = jax.random.normal(jax.random.fold_in(key, 71), (HEADS * HEAD, D), jnp.float32)
    return jnp.clip(base * 2.0, -12.0, 12.0).astype(jnp.bfloat16)


def steps_of(stream_key, shape, cuts, least, largest):
    def one(axis_at, blocks):
        steps = jax.random.uniform(jax.random.fold_in(jax.random.fold_in(stream_key, 6), axis_at), (blocks,), jnp.float32, least / len(cuts), largest / len(cuts))
        return jnp.repeat(jnp.exp(steps), shape[axis_at] // blocks).reshape((-1,) + (1,) * (len(shape) - axis_at - 1))

    factor_of = one(*cuts[0])
    for cut in cuts[1:]:
        factor_of = factor_of * one(*cut)
    return factor_of


def centred(rng, shape, spread, limit, shards=(), held_as=jnp.bfloat16):
    factor_of = steps_of(rng, shape, shards, -0.22, 0.18) if shards else 1.0
    array = jax.random.normal(rng, shape, jnp.float32) * spread * factor_of
    return jnp.minimum(jnp.maximum(array, -limit), limit).astype(held_as)


def setup_inputs(seed: int = 0) -> dict:
    splits = jax.random.split(jax.random.key(seed), 12)
    return {
        "queries": draw_queries(jax.random.fold_in(splits[11], 71), 0),
        "keys": draw_keys(jax.random.fold_in(splits[11], 71), 0),
        "values": centred(splits[2], (TOKENS, KV_WIDTH), 1.0, 6.0, ((0, 16), (1, 2))),
        "q_gain": draw_q_gain(jax.random.fold_in(splits[11], 71), 0),
        "k_gain": draw_k_gain(jax.random.fold_in(splits[11], 71), 0),
        "w_out": draw_w_out(jax.random.fold_in(splits[11], 71), 0),
        "residual": centred(splits[6], (TOKENS, D), 1.0, 6.0, ((0, 32),)),
        "norm_gain": jnp.clip(1.0 + 0.18 * jax.random.normal(splits[7], (D,), jnp.float32), 0.1, 1.9),
        "w_gate": centred(splits[8], (D, FF), D ** -0.5, 0.125, ((0, 16), (1, 2))),
        "w_up": centred(splits[9], (D, FF), D ** -0.5, 0.125, ((0, 16), (1, 2))),
        "w_down": centred(splits[10], (FF, D), (FF // 9) ** -0.5, 0.25, ((0, 2), (1, 16))),
    }


EPS = 1e-06
THETA = 10000.0

def turn_half(part, angle):
    quarter = part.shape[-1] // 2
    cos_table = jnp.cos(angle)[:, None, :]
    sin_table = jnp.sin(angle)[:, None, :]
    first_part = part[..., :quarter]
    second_part = part[..., quarter:]
    return jnp.concatenate([first_part * cos_table - second_part * sin_table, first_part * sin_table + second_part * cos_table], axis=-1)

def head_norm_rope(flat, gain, offset, head_count):
    tok_rows = flat.shape[0]
    head_size = flat.shape[1] // head_count
    heads = flat.astype(jnp.float32).reshape(tok_rows, head_count, head_size)
    heads = heads * lax.rsqrt(lax.optimization_barrier(jnp.mean(heads * heads, axis=-1, keepdims=True)) + EPS) * gain.astype(jnp.float32)
    positions = offset + jnp.arange(tok_rows, dtype=jnp.int32)
    row_pos = (positions // GRID_W).astype(jnp.float32)
    col_pos = (positions % GRID_W).astype(jnp.float32)
    half_size = head_size // 2
    inv_freq = THETA ** (-jnp.arange(0, half_size, 2, dtype=jnp.float32) / half_size)
    turned = jnp.concatenate([turn_half(heads[..., :half_size], row_pos[:, None] * inv_freq[None, :]), turn_half(heads[..., half_size:], col_pos[:, None] * inv_freq[None, :])], axis=-1)
    return turned.reshape(tok_rows, head_count * head_size).astype(jnp.bfloat16)

def reference(queries, keys, values, q_gain, k_gain, w_out, residual, norm_gain, w_gate, w_up, w_down):
    q_group = HEADS // KV_HEADS
    q_rot = head_norm_rope(queries, q_gain, 0, HEADS)
    k_rot = head_norm_rope(keys, k_gain, 0, KV_HEADS)
    key_heads = k_rot.reshape(TOKENS, KV_HEADS, HEAD).astype(jnp.float32)
    value_heads = values.reshape(TOKENS, KV_HEADS, HEAD).astype(jnp.float32)
    block_len = math.gcd(TOKENS, 256)
    query_blocks = q_rot.reshape(TOKENS // block_len, block_len, KV_HEADS, q_group, HEAD)
    score_scale = HEAD ** (-0.5)

    def attend_block(query_block):
        scores = jnp.einsum('qhgd,khd->hgqk', query_block.astype(jnp.float32), key_heads) * score_scale
        top = lax.optimization_barrier(jnp.max(scores, axis=-1, keepdims=True))
        weights = jnp.exp(scores - top)
        totals = lax.optimization_barrier(jnp.sum(weights, axis=-1))
        rounded = weights.astype(jnp.bfloat16).astype(jnp.float32)
        mixed = jnp.einsum('hgqk,khd->qhgd', rounded, value_heads)
        mixed = mixed / jnp.transpose(totals, (2, 0, 1))[..., None]
        return mixed.astype(jnp.bfloat16).reshape(block_len, ATTN)
    attn = lax.map(attend_block, query_blocks).reshape(TOKENS, ATTN)
    proj = jnp.dot(attn, w_out, preferred_element_type=jnp.float32)
    mid = residual.astype(jnp.float32) + proj
    normed = (mid * lax.rsqrt(lax.optimization_barrier(jnp.mean(mid * mid, axis=-1, keepdims=True)) + EPS) * norm_gain.astype(jnp.float32)).astype(jnp.bfloat16)
    gate = jnp.dot(normed, w_gate, preferred_element_type=jnp.float32)
    up_part = jnp.dot(normed, w_up, preferred_element_type=jnp.float32)
    hidden = (jax.nn.silu(gate) * up_part).astype(jnp.bfloat16)
    down = jnp.dot(hidden, w_down, preferred_element_type=jnp.float32)
    return (mid + 0.5 * down).astype(jnp.bfloat16)
```

```python
import functools

import jax
import jax.numpy as jnp
import numpy as np
from jax import lax
from jax.experimental import pallas as pl
from jax.experimental.pallas import tpu as pltpu
from jax.sharding import Mesh
from jax.sharding import PartitionSpec as P

GRID_W = 128


EPS = 1e-06
THETA = 10000.0


def rope_tables(offset, rows, head_size, copies):
    half_size = head_size // 2
    quarter = half_size // 2
    inv_freq = THETA ** (-jnp.arange(0, half_size, 2, dtype=jnp.float32) / half_size)
    positions = offset + jnp.arange(rows, dtype=jnp.int32)
    row_angle = (positions // GRID_W).astype(jnp.float32)[:, None] * inv_freq[None, :]
    col_angle = (positions % GRID_W).astype(jnp.float32)[:, None] * inv_freq[None, :]
    angle = jnp.concatenate([row_angle, row_angle, col_angle, col_angle] * copies, axis=1)
    sign = np.where(np.arange(head_size * copies) % half_size < quarter, -1.0, 1.0)
    return jnp.cos(angle), jnp.sin(angle) * sign.astype(np.float32)


def prep_kernel(qkv_ref, cos_ref, sin_ref, qg_ref, kg_ref, q_out, kv_out, *, head_size, group):
    width = 2 * head_size
    quarter = head_size // 4
    lane = lax.broadcasted_iota(jnp.int32, (1, width), 1)
    low = lane < head_size
    first = (lane % (2 * quarter)) < quarter
    cos_table = cos_ref[...]
    sin_table = sin_ref[...]

    def turn(pair, gain):
        square = pair * pair
        low_mean = jnp.sum(jnp.where(low, square, 0.0), axis=-1, keepdims=True) / head_size
        high_mean = jnp.sum(jnp.where(low, 0.0, square), axis=-1, keepdims=True) / head_size
        scale = jnp.where(low, lax.rsqrt(low_mean + EPS), lax.rsqrt(high_mean + EPS))
        pair = pair * scale * gain
        ahead = pltpu.roll(pair, width - quarter, 1)
        behind = pltpu.roll(pair, quarter, 1)
        return pair * cos_table + jnp.where(first, ahead, behind) * sin_table

    for at in range(group // 2):
        pair = turn(qkv_ref[:, at * width : (at + 1) * width].astype(jnp.float32), qg_ref[...])
        pair = pair * head_size ** (-0.5)
        q_out[2 * at] = jnp.where(low, pair, 0.0).astype(jnp.bfloat16)
        q_out[2 * at + 1] = jnp.where(low, pltpu.roll(pair, head_size, 1), 0.0).astype(jnp.bfloat16)
    raw = qkv_ref[:, group * head_size :].astype(jnp.float32)
    turned = turn(raw, kg_ref[...])
    kv_out[...] = jnp.where(low, turned, raw).astype(jnp.bfloat16)


def attend_kernel(q_ref, kv_ref, out_ref, *, head_size, group):
    width = 2 * head_size
    lane = lax.broadcasted_iota(jnp.int32, (1, width), 1)
    kv = kv_ref[...]
    mixed = []
    for head in range(group):
        scores = lax.dot_general(
            q_ref[head], kv, (((1,), (1,)), ((), ())), preferred_element_type=jnp.float32
        )
        top = jnp.max(scores, axis=-1, keepdims=True)
        weights = jnp.exp(scores - top)
        totals = jnp.sum(weights, axis=-1, keepdims=True)
        mix = jnp.dot(weights.astype(jnp.bfloat16), kv, preferred_element_type=jnp.float32)
        mixed.append(mix / totals)
    for at in range(group // 2):
        pair = jnp.where(
            lane < head_size, pltpu.roll(mixed[2 * at], head_size, 1), mixed[2 * at + 1]
        )
        out_ref[:, at * width : (at + 1) * width] = pair.astype(jnp.bfloat16)


def attention(packed, offset, q_gain, k_gain, outer):
    rows, total = packed.shape
    head_size = q_gain.shape[0]
    group = total // head_size - 2
    width = 2 * head_size
    cos_table, sin_table = rope_tables(offset, rows, head_size, 2)
    twice = lambda gain: jnp.concatenate([gain, gain])[None, :]
    q_rot, kv = pl.pallas_call(
        functools.partial(prep_kernel, head_size=head_size, group=group),
        out_shape=(
            jax.ShapeDtypeStruct((group, rows, width), jnp.bfloat16),
            jax.ShapeDtypeStruct((rows, width), jnp.bfloat16),
        ),
    )(packed, cos_table, sin_table, twice(q_gain), twice(k_gain))
    kv_all = lax.all_gather(kv, outer, axis=0, tiled=True)
    block = rows
    while block > 256 or rows % block:
        block -= 8
    return pl.pallas_call(
        functools.partial(attend_kernel, head_size=head_size, group=group),
        grid=(rows // block,),
        in_specs=[
            pl.BlockSpec((group, block, width), lambda i: (0, i, 0)),
            pl.BlockSpec(kv_all.shape, lambda i: (0, 0)),
        ],
        out_specs=pl.BlockSpec((block, group * head_size), lambda i: (i, 0)),
        out_shape=jax.ShapeDtypeStruct((rows, group * head_size), jnp.bfloat16),
    )(q_rot, kv_all)


def swap(array, step):
    axis, size, bit = step
    return lax.ppermute(array, axis, [(i, i ^ bit) for i in range(size)])


def bits_of(axis, size):
    return [(axis, size, 1 << b) for b in reversed(range(size.bit_length() - 1))]


def make_body(sizes):
    hi, lo, inner, tp = (sizes[n] for n in ("h", "l", "m", "t"))
    members = lo * inner * tp
    steps = bits_of("t", tp) + bits_of("l", lo) + bits_of("m", inner)
    near, far = steps[-1:], steps[:-1]

    def body(queries, keys, values, q_gain, k_gain, w_out, residual, norm_gain, w_gate, w_up, w_down):
        tok_rows = queries.shape[0]
        head_size = q_gain.shape[0]
        own = residual.shape[0]
        features = residual.shape[1]
        split = lambda a: a.reshape(tok_rows, inner, a.shape[1] // inner)
        packed = jnp.concatenate([split(queries), split(keys), split(values)], axis=2)
        packed = lax.all_to_all(packed, "m", split_axis=1, concat_axis=0, tiled=True)
        packed = packed.reshape(inner * tok_rows, packed.shape[2])
        block_at = lax.axis_index("h") * lo + lax.axis_index("l")

        out_full = lax.all_gather(w_out, "t", axis=0, tiled=True)
        place = lambda w: lax.all_to_all(w, ("l", "m"), split_axis=1, concat_axis=0, tiled=True)
        gate_w = lax.all_gather(place(w_gate), "h", axis=0, tiled=True)
        up_w = lax.all_gather(place(w_up), "h", axis=0, tiled=True)
        down_w = lax.all_to_all(w_down, ("l", "m"), split_axis=0, concat_axis=1, tiled=True)
        down_w = lax.all_gather(down_w, "h", axis=1, tiled=True)

        attn = attention(packed, block_at * inner * tok_rows, q_gain, k_gain, ("h", "l"))
        width = attn.shape[1]
        columns = lax.all_to_all(
            attn.reshape(inner * tp, own, width), ("m", "t"), split_axis=0, concat_axis=0, tiled=True
        )
        columns = columns.reshape(inner, tp, own, width).transpose(2, 1, 0, 3)
        columns = columns.reshape(own, tp * inner * width)
        proj = jnp.dot(columns, out_full, preferred_element_type=jnp.float32)
        mid = residual.astype(jnp.float32) + proj
        normed = (
            mid * lax.rsqrt(jnp.mean(mid * mid, axis=-1, keepdims=True) + EPS) * norm_gain
        ).astype(jnp.bfloat16)

        parts = 3 if own % 24 == 0 else 1
        each = own // parts
        downs = []
        for part in range(parts):
            turn = part % len(far)
            order = far[turn:] + far[:turn] + near
            rows = normed[part * each : (part + 1) * each]
            for step in order:
                rows = jnp.concatenate([rows, swap(rows, step)], axis=0)
            gate = jnp.dot(rows, gate_w, preferred_element_type=jnp.float32)
            up_part = jnp.dot(rows, up_w, preferred_element_type=jnp.float32)
            hidden = (jax.nn.silu(gate) * up_part).astype(jnp.bfloat16)
            terms = jnp.dot(hidden, down_w, preferred_element_type=jnp.float32)
            for step in reversed(order):
                keep = terms.shape[0] // 2
                sent = swap(terms[keep:].astype(jnp.bfloat16), step)
                terms = terms[:keep].astype(jnp.float32) + sent.astype(jnp.float32)
            downs.append(terms)
        down = jnp.concatenate(downs, axis=0)
        return (mid + 0.5 * down).astype(jnp.bfloat16)

    return body


def solution(mesh):
    sp, tp = mesh.shape["sp"], mesh.shape["tp"]

    def whole(queries, keys, values, q_gain, *rest):
        kv_local = keys.shape[1] // (q_gain.shape[0] * tp)
        inner = kv_local
        lo = max(1, 16 // (tp * inner))
        hi = sp // (lo * inner)
        grid = Mesh(mesh.devices.reshape(hi, lo, inner, tp), ("h", "l", "m", "t"))
        s = ("h", "l", "m")
        return jax.shard_map(
            make_body(dict(grid.shape)),
            mesh=grid,
            in_specs=(
                P(s, "t"),
                P(s, "t"),
                P(s, "t"),
                P(),
                P(),
                P("t", None),
                P(s + ("t",), None),
                P(),
                P(s, "t"),
                P(s, "t"),
                P("t", s),
            ),
            out_specs=P(s + ("t",), None),
            check_vma=False,
        )(queries, keys, values, q_gain, *rest)

    return whole
```

```python
import functools

import jax
import jax.numpy as jnp
import numpy as np
from jax import lax
from jax.experimental import pallas as pl
from jax.experimental.pallas import tpu as pltpu
from jax.sharding import Mesh
from jax.sharding import PartitionSpec as P

GRID_W = 128


EPS = 1e-06
THETA = 10000.0


def rope_tables(offset, rows, head_size, copies):
    half_size = head_size // 2
    quarter = half_size // 2
    inv_freq = THETA ** (-jnp.arange(0, half_size, 2, dtype=jnp.float32) / half_size)
    positions = offset + jnp.arange(rows, dtype=jnp.int32)
    row_angle = (positions // GRID_W).astype(jnp.float32)[:, None] * inv_freq[None, :]
    col_angle = (positions % GRID_W).astype(jnp.float32)[:, None] * inv_freq[None, :]
    angle = jnp.concatenate([row_angle, row_angle, col_angle, col_angle] * copies, axis=1)
    sign = np.where(np.arange(head_size * copies) % half_size < quarter, -1.0, 1.0)
    return jnp.cos(angle), jnp.sin(angle) * sign.astype(np.float32)


def prep_kernel(qkv_ref, cos_ref, sin_ref, qg_ref, kg_ref, q_out, kv_out, *, head_size, group):
    width = 2 * head_size
    quarter = head_size // 4
    lane = lax.broadcasted_iota(jnp.int32, (1, width), 1)
    low = lane < head_size
    first = (lane % (2 * quarter)) < quarter
    cos_table = cos_ref[...]
    sin_table = sin_ref[...]

    def turn(pair, gain):
        square = pair * pair
        low_mean = jnp.sum(jnp.where(low, square, 0.0), axis=-1, keepdims=True) / head_size
        high_mean = jnp.sum(jnp.where(low, 0.0, square), axis=-1, keepdims=True) / head_size
        scale = jnp.where(low, lax.rsqrt(low_mean + EPS), lax.rsqrt(high_mean + EPS))
        pair = pair * scale * gain
        ahead = pltpu.roll(pair, width - quarter, 1)
        behind = pltpu.roll(pair, quarter, 1)
        return pair * cos_table + jnp.where(first, ahead, behind) * sin_table

    for at in range(group // 2):
        pair = turn(qkv_ref[:, at * width : (at + 1) * width].astype(jnp.float32), qg_ref[...])
        pair = pair * head_size ** (-0.5)
        q_out[2 * at] = jnp.where(low, pair, 0.0).astype(jnp.bfloat16)
        q_out[2 * at + 1] = jnp.where(low, pltpu.roll(pair, head_size, 1), 0.0).astype(jnp.bfloat16)
    raw = qkv_ref[:, group * head_size :].astype(jnp.float32)
    turned = turn(raw, kg_ref[...])
    kv_out[...] = jnp.where(low, turned, raw).astype(jnp.bfloat16)


def attend_kernel(q_ref, kv_ref, out_ref, *, head_size, group):
    width = 2 * head_size
    lane = lax.broadcasted_iota(jnp.int32, (1, width), 1)
    kv = kv_ref[...]
    mixed = []
    for head in range(group):
        scores = lax.dot_general(
            q_ref[head], kv, (((1,), (1,)), ((), ())), preferred_element_type=jnp.float32
        )
        top = jnp.max(scores, axis=-1, keepdims=True)
        weights = jnp.exp(scores - top)
        totals = jnp.sum(weights, axis=-1, keepdims=True)
        mix = jnp.dot(weights.astype(jnp.bfloat16), kv, preferred_element_type=jnp.float32)
        mixed.append(mix / totals)
    for at in range(group // 2):
        pair = jnp.where(
            lane < head_size, pltpu.roll(mixed[2 * at], head_size, 1), mixed[2 * at + 1]
        )
        out_ref[:, at * width : (at + 1) * width] = pair.astype(jnp.bfloat16)


def attention(packed, offset, q_gain, k_gain, outer):
    rows, total = packed.shape
    head_size = q_gain.shape[0]
    group = total // head_size - 2
    width = 2 * head_size
    cos_table, sin_table = rope_tables(offset, rows, head_size, 2)
    twice = lambda gain: jnp.concatenate([gain, gain])[None, :]
    prep = pl.pallas_call(
        functools.partial(prep_kernel, head_size=head_size, group=group),
        out_shape=(
            jax.ShapeDtypeStruct((group, rows, width), jnp.bfloat16),
            jax.ShapeDtypeStruct((rows, width), jnp.bfloat16),
        ),
    )
    q_rot, kv = prep(packed, cos_table, sin_table, twice(q_gain), twice(k_gain))
    kv_all = kv
    for step in outer:
        kv_all = jnp.concatenate([kv_all, swap(kv_all, step)], axis=0)
    block = rows
    while block > 256 or rows % block:
        block -= 8
    return pl.pallas_call(
        functools.partial(attend_kernel, head_size=head_size, group=group),
        grid=(rows // block,),
        in_specs=[
            pl.BlockSpec((group, block, width), lambda i: (0, i, 0)),
            pl.BlockSpec(kv_all.shape, lambda i: (0, 0)),
        ],
        out_specs=pl.BlockSpec((block, group * head_size), lambda i: (i, 0)),
        out_shape=jax.ShapeDtypeStruct((rows, group * head_size), jnp.bfloat16),
    )(q_rot, kv_all)


def swap(array, step):
    axis, size, bit = step
    return lax.ppermute(array, axis, [(i, i ^ bit) for i in range(size)])


def bits_of(axis, size):
    return [(axis, size, 1 << b) for b in reversed(range(size.bit_length() - 1))]


def relative(array, axis, size):
    if size == 1:
        return array
    pieces = array.reshape(array.shape[0], size, array.shape[1] // size)
    here = lax.axis_index(axis)
    out = [lax.dynamic_index_in_dim(pieces, here ^ r, 1, keepdims=False) for r in range(size)]
    return jnp.concatenate(out, axis=1)


def make_body(sizes):
    hi, lo, inner, tp = (sizes[n] for n in ("h", "l", "m", "t"))
    steps = bits_of("t", tp) + bits_of("l", lo) + bits_of("m", inner)
    near, far = steps[-1:], steps[:-1]

    def body(queries, keys, values, q_gain, k_gain, w_out, residual, norm_gain, w_gate, w_up, w_down):
        tok_rows = queries.shape[0]
        own = residual.shape[0]
        cut = lambda w: w.reshape(w.shape[0], lo * inner, w.shape[1] // (lo * inner))
        split = lambda a: a.reshape(tok_rows, inner, a.shape[1] // inner)
        packed = jnp.concatenate([split(queries), split(keys), split(values)], axis=2)
        packed = lax.all_to_all(packed, "m", split_axis=1, concat_axis=0, tiled=True)
        packed = packed.reshape(inner * tok_rows, packed.shape[2])
        block_at = lax.axis_index("h") * lo + lax.axis_index("l")

        out_rel = w_out
        for step in bits_of("t", tp)[::-1]:
            out_rel = jnp.concatenate([out_rel, swap(out_rel, step)], axis=0)
        gate_up = jnp.concatenate([cut(w_gate), cut(w_up)], axis=2)
        gate_up, w_down, packed = lax.optimization_barrier((gate_up, w_down, packed))
        gate_up = lax.all_to_all(gate_up, ("l", "m"), split_axis=1, concat_axis=0, tiled=True)
        gate_up = gate_up.reshape(gate_up.shape[0], gate_up.shape[2])
        down_w = lax.all_to_all(w_down, ("l", "m"), split_axis=0, concat_axis=1, tiled=True)
        for step in bits_of("h", hi)[::-1]:
            gate_up = jnp.concatenate([gate_up, swap(gate_up, step)], axis=0)
        for step in bits_of("h", hi)[::-1]:
            down_w = jnp.concatenate([down_w, swap(down_w, step)], axis=1)
        units = gate_up.shape[1] // 2

        attn = attention(packed, block_at * inner * tok_rows, q_gain, k_gain, bits_of("h", hi) + bits_of("l", lo))
        width = attn.shape[1]
        pieces = attn.reshape(inner * tp, own, width)
        columns = lax.all_to_all(pieces, ("m", "t"), split_axis=0, concat_axis=0, tiled=True)
        columns = columns.reshape(inner, tp, own, width).transpose(2, 1, 0, 3)
        columns = relative(columns.reshape(own, tp * inner * width), "t", tp)
        proj = jnp.dot(columns, out_rel, preferred_element_type=jnp.float32)
        mid = residual.astype(jnp.float32) + proj
        normed = (
            mid * lax.rsqrt(jnp.mean(mid * mid, axis=-1, keepdims=True) + EPS) * norm_gain
        ).astype(jnp.bfloat16)
        normed = relative(normed, "h", hi)

        parts = 3 if own % 24 == 0 else 1
        each = own // parts
        downs = []
        for part in range(parts):
            turn = part % len(far)
            order = far[turn:] + far[:turn] + near
            rows = normed[part * each : (part + 1) * each]
            for step in order:
                rows = jnp.concatenate([rows, swap(rows, step)], axis=0)
            both = jnp.dot(rows, gate_up, preferred_element_type=jnp.float32)
            gate, up_part = both[:, :units], both[:, units:]
            hidden = (jax.nn.silu(gate) * up_part).astype(jnp.bfloat16)
            terms = jnp.dot(hidden, down_w, preferred_element_type=jnp.float32).astype(jnp.bfloat16)
            for step in reversed(order):
                keep = terms.shape[0] // 2
                sent = swap(terms[keep:].astype(jnp.bfloat16), step)
                terms = terms[:keep].astype(jnp.float32) + sent.astype(jnp.float32)
            downs.append(terms)
        down = relative(jnp.concatenate(downs, axis=0), "h", hi)
        return (mid + 0.5 * down).astype(jnp.bfloat16)

    return body


def solution(mesh):
    sp, tp = mesh.shape["sp"], mesh.shape["tp"]

    def whole(queries, keys, values, q_gain, *rest):
        kv_local = keys.shape[1] // (q_gain.shape[0] * tp)
        inner = kv_local
        lo = max(1, 16 // (tp * inner))
        hi = sp // (lo * inner)
        grid = Mesh(mesh.devices.reshape(hi, lo, inner, tp), ("h", "l", "m", "t"))
        s = ("h", "l", "m")
        step = jax.shard_map(
            make_body(dict(grid.shape)),
            mesh=grid,
            in_specs=(
                P(s, "t"),
                P(s, "t"),
                P(s, "t"),
                P(),
                P(),
                P("t", None),
                P(s + ("t",), None),
                P(),
                P(s, "t"),
                P(s, "t"),
                P("t", s),
            ),
            out_specs=P(s + ("t",), None),
            check_vma=False,
        )
        return step(queries, keys, values, q_gain, *rest)

    return whole
```
